32 devices in a mesh: sp: 4 (over z), fs: 4 (over y, x), tp: 2 (over core).
Axes of the slice: x: 2, y: 2, z: 4, core: 2. Of those that a mesh axis runs over, the one named last changes fastest.
Arguments:
- tokens: bfloat16 [1024, 2048], P('sp', ('fs', 'tp')), may hold values from -500 to 500
- norm_gain: float32 [2048], replicated, may hold values from 0.1 to 1.9
- query_w: bfloat16 [2048, 1024], P('sp', ('fs', 'tp')), may hold values from -1 to 1
- key_w: bfloat16 [2048, 512], P('sp', ('fs', 'tp')), may hold values from -1 to 1
- value_w: bfloat16 [2048, 512], P('sp', ('fs', 'tp')), may hold values from -0.125 to 0.125
- recept_w: bfloat16 [2048, 1024], P('sp', ('fs', 'tp')), may hold values from -0.125 to 0.125
- rec_key_w: bfloat16 [2048, 1024], P('sp', ('fs', 'tp')), may hold values from -0.125 to 0.125
- rec_value_w: bfloat16 [2048, 1024], P('sp', ('fs', 'tp')), may hold values from -0.125 to 0.125
- decay_down: bfloat16 [2048, 64], replicated, may hold values from -0.125 to 0.125
- decay_up: bfloat16 [64, 1024], replicated, may hold values from -1 to 1
- decay_base: float32 [16, 1024], P(('fs', 'tp'), 'sp'), may hold values from -14 to 0
- learn_rate: float32 [1024], P(('fs', 'tp')), may hold values from 0.1 to 1
- query_gain: float32 [64], replicated, may hold values from 0 to 7
- key_gain: float32 [64], replicated, may hold values from 0 to 7
- sink_logit: float32 [16], P(('fs', 'tp')), may hold values from 1 to 5
- group_gain: float32 [1024], P(('fs', 'tp')), may hold values from 0.1 to 1.9
- out_att_w: bfloat16 [1024, 2048], P(('fs', 'tp'), 'sp'), may hold values from -0.75 to 0.75
- out_rec_w: bfloat16 [1024, 2048], P(('fs', 'tp'), 'sp'), may hold values from -0.1875 to 0.1875
Outputs:
- mixed: bfloat16 [1024, 2048], P(('sp', 'fs', 'tp'))
- row_lse: float32 [16, 1024], P(('fs', 'tp'), 'sp')
The draws below stay inside these ranges and needn't reach their ends.
All inputs are finite; a program needn't handle non-finite values.
Results may differ from the reference program's by a relative error of at most 0.015.
Values may be sent and summed in bfloat16 or wider, within the bound.
A program may use at most 64 MiB of HBM per device.

```python
import math
import jax
import jax.numpy as jnp
from jax import lax

D = 2048
HEAD = 64
ATT_HEADS = 16
KV_HEADS = 8
RECURRENT_HEADS = 16
DECAY_RANK = 64
WINDOW = 128
TOK = 256
SEQUENCE_LENGTH = 1024
ATT_WIDTH = 1024
KV_WIDTH = 512
REC_WIDTH = 1024
N_FS = 4
N_TP = 2


def draw_tokens(key, part):
    normal_key = jax.random.fold_in(key, 101)
    base_values = jnp.clip(jax.random.normal(normal_key, (SEQUENCE_LENGTH, D), jnp.float32), -5.0, 5.0)
    column_scale = jnp.exp(jnp.log(10.0) * jnp.arange(D, dtype=jnp.float32) / D)
    row_scale = jnp.exp(jax.random.uniform(jax.random.fold_in(key, 102), (SEQUENCE_LENGTH, 1), jnp.float32, 0.0, 2.3))
    return (base_values * column_scale[None, :] * row_scale).astype(jnp.bfloat16)


def draw_head_gain(key, salt):
    gain_key = jax.random.fold_in(key, salt)
    gain_vec = 1.0 + 0.18 * jnp.clip(jax.random.normal(gain_key, (HEAD,), jnp.float32), -4.5, 4.5)
    return gain_vec


def draw_query_gain(key, part):
    return draw_head_gain(key, 103)


def draw_key_gain(key, part):
    return draw_head_gain(key, 104)


def draw_attention_pair(key):
    scale_val = 1.0 / jnp.sqrt(jnp.float32(D))
    query_part = jnp.clip(jax.random.normal(jax.random.fold_in(key, 201), (D, ATT_WIDTH), jnp.float32), -5.0, 5.0) * scale_val
    key_part = jnp.clip(jax.random.normal(jax.random.fold_in(key, 202), (D, KV_WIDTH), jnp.float32), -5.0, 5.0) * scale_val
    return (query_part, key_part)


def draw_query_w(key, part):
    return draw_attention_pair(key)[0].astype(jnp.bfloat16)


def draw_key_w(key, part):
    return draw_attention_pair(key)[1].astype(jnp.bfloat16)


def draw_decay_base(key, part):
    fast_share = 0.5
    fast_heads = jax.random.uniform(jax.random.fold_in(key, 301), (RECURRENT_HEADS, 1), jnp.float32) < fast_share
    head_rate = jnp.where(fast_heads, 1.0 / 40.0, 0.4 / SEQUENCE_LENGTH)
    block_factor = jnp.exp(jax.random.uniform(jax.random.fold_in(key, 302), (RECURRENT_HEADS, SEQUENCE_LENGTH // TOK), jnp.float32, -0.7, 0.7))
    steady_frequency = head_rate * jnp.repeat(block_factor, TOK, axis=1)
    spike_locations = jax.random.randint(jax.random.fold_in(key, 303), (3,), 0, SEQUENCE_LENGTH)
    spike_frequency = jnp.exp(jax.random.uniform(jax.random.fold_in(key, 304), (RECURRENT_HEADS, 3), jnp.float32, -1.9, -0.7))
    token_places = jnp.arange(SEQUENCE_LENGTH)
    spike_events = token_places[None, None, :] == spike_locations[None, :, None]
    spike_pattern = jnp.sum(jnp.where(spike_events, spike_frequency[:, :, None], 0.0), axis=1)
    combined_frequency = jnp.where(spike_pattern > 0.0, spike_pattern, steady_frequency)
    return jnp.log(combined_frequency)


def block_levels(stream_key, dims, shards, low, high):
    factor_of = 1.0
    for axis_at, shards_of in shards:
        steps = jax.random.uniform(jax.random.fold_in(jax.random.fold_in(stream_key, 6), axis_at), (shards_of,), jnp.float32, low / len(shards), high / len(shards))
        factor_of = factor_of * jnp.repeat(jnp.exp(steps), dims[axis_at] // shards_of).reshape((-1,) + (1,) * (len(dims) - 1 - axis_at))
    return factor_of


def gaussian(rng, shape, deviation, limit, split=(), kind=jnp.bfloat16):
    result = jax.random.normal(rng, shape, jnp.float32) * deviation
    if len(split) > 0:
        result = block_levels(rng, shape, split, -0.22, 0.18) * result
    return jnp.clip(result, min=-limit, max=limit).astype(kind)


def setup_inputs(seed: int = 0) -> dict:
    seeds = jax.random.split(jax.random.key(seed), 19)
    return {
        "tokens": draw_tokens(jax.random.fold_in(seeds[18], 71), 0),
        "norm_gain": jnp.clip(1.0 + 0.18 * jax.random.normal(seeds[1], (D,), jnp.float32), 0.1, 1.9),
        "query_w": draw_query_w(jax.random.fold_in(seeds[18], 71), 0),
        "key_w": draw_key_w(jax.random.fold_in(seeds[18], 71), 0),
        "value_w": gaussian(seeds[4], (D, KV_WIDTH), D ** -0.5, 0.125, ((0, 4), (1, 8))),
        "recept_w": gaussian(seeds[5], (D, REC_WIDTH), D ** -0.5, 0.125, ((0, 4), (1, 8))),
        "rec_key_w": gaussian(seeds[6], (D, REC_WIDTH), D ** -0.5, 0.125, ((0, 4), (1, 8))),
        "rec_value_w": gaussian(seeds[7], (D, REC_WIDTH), D ** -0.5, 0.125, ((0, 4), (1, 8))),
        "decay_down": gaussian(seeds[8], (D, DECAY_RANK), D ** -0.5, 0.125),
        "decay_up": gaussian(seeds[9], (DECAY_RANK, REC_WIDTH), (DECAY_RANK // 2) ** -0.5, 1.0),
        "decay_base": draw_decay_base(jax.random.fold_in(seeds[18], 71), 0),
        "learn_rate": jnp.clip(0.1 + 0.9 * jax.random.uniform(seeds[11], (REC_WIDTH,), jnp.float32) ** block_levels(seeds[11], (REC_WIDTH,), ((0, 8),), -0.2, 0.2), 0.1, 1.0),
        "query_gain": draw_query_gain(jax.random.fold_in(seeds[18], 71), 0),
        "key_gain": draw_key_gain(jax.random.fold_in(seeds[18], 71), 0),
        "sink_logit": jnp.clip(1.0 + 4.0 * jax.random.uniform(seeds[14], (ATT_HEADS,), jnp.float32) ** block_levels(seeds[14], (ATT_HEADS,), ((0, 8),), -0.2, 0.2), 1.0, 5.0),
        "group_gain": jnp.clip(1.0 + 0.18 * jax.random.normal(seeds[15], (REC_WIDTH,), jnp.float32), 0.1, 1.9),
        "out_att_w": gaussian(seeds[16], (ATT_WIDTH, D), (ATT_WIDTH // 16) ** -0.5, 0.75, ((0, 8), (1, 4))),
        "out_rec_w": gaussian(seeds[17], (REC_WIDTH, D), REC_WIDTH ** -0.5, 0.1875, ((0, 8), (1, 4))),
    }


NORM_EPS = 1e-06
KEY_EPS = 1e-06
GROUP_EPS = 0.00064
EXACT_PRECISION = lax.Precision.HIGHEST

def project(hidden, weight_mat):
    product = jnp.dot(hidden, weight_mat, preferred_element_type=jnp.float32)
    return lax.optimization_barrier(product.astype(jnp.bfloat16))

def head_rms(values, gain_vec, num_heads):
    shaped = values.astype(jnp.float32).reshape(values.shape[0], num_heads, HEAD)
    mean_sq = lax.optimization_barrier(jnp.mean(shaped * shaped, axis=-1, keepdims=True))
    normed = (shaped * lax.rsqrt(mean_sq + NORM_EPS) * gain_vec).astype(jnp.bfloat16)
    return lax.optimization_barrier(normed)

def window_head(query_head, key_head, value_head, sink_value):
    blocks = query_head.shape[0] // WINDOW
    query_blocks = query_head.astype(jnp.float32).reshape(blocks, WINDOW, HEAD)
    key_blocks = key_head.astype(jnp.float32).reshape(blocks, WINDOW, HEAD)
    value_blocks = value_head.astype(jnp.float32).reshape(blocks, WINDOW, HEAD)
    zero_block = jnp.zeros((1, WINDOW, HEAD), jnp.float32)
    key_band = jnp.concatenate([jnp.concatenate([zero_block, key_blocks[:-1]], axis=0), key_blocks], axis=1)
    value_band = jnp.concatenate([jnp.concatenate([zero_block, value_blocks[:-1]], axis=0), value_blocks], axis=1)
    scores = jnp.einsum('nqd,nsd->nqs', query_blocks, key_band) * (1.0 / math.sqrt(HEAD))
    lag_table = jnp.arange(WINDOW)[:, None] + WINDOW - jnp.arange(2 * WINDOW)[None, :]
    key_place = (jnp.arange(blocks)[:, None] - 1) * WINDOW + jnp.arange(2 * WINDOW)[None, :]
    allowed = ((lag_table >= 0) & (lag_table < WINDOW))[None, :, :] & (key_place >= 0)[:, None, :]
    masked = jnp.where(allowed, scores, -jnp.inf)
    row_top = jnp.maximum(lax.optimization_barrier(jnp.max(masked, axis=-1, keepdims=True)), sink_value)
    weight = jnp.where(allowed, jnp.exp(masked - row_top), 0.0)
    row_total = lax.optimization_barrier(jnp.sum(weight, axis=-1, keepdims=True)) + jnp.exp(sink_value - row_top)
    head_lse = (row_top + jnp.log(row_total)).reshape(-1)
    att_probs = lax.optimization_barrier((weight / row_total).astype(jnp.bfloat16)).astype(jnp.float32)
    head_out = jnp.einsum('nqs,nsd->nqd', att_probs, value_band).reshape(-1, HEAD)
    return (head_out.astype(jnp.bfloat16), head_lse)

def attention(query_n, key_n, att_values, sink_logit):
    group_size = ATT_HEADS // KV_HEADS
    query_heads = query_n.transpose(1, 0, 2)
    key_heads = jnp.repeat(key_n.transpose(1, 0, 2), group_size, axis=0)
    value_heads = jnp.repeat(att_values.reshape(SEQUENCE_LENGTH, KV_HEADS, HEAD).transpose(1, 0, 2), group_size, axis=0)
    head_outs, head_lse = lax.map(lambda packed: window_head(*packed), (query_heads, key_heads, value_heads, sink_logit))
    return (head_outs.transpose(1, 0, 2).reshape(SEQUENCE_LENGTH, ATT_WIDTH), head_lse)

def recurrence(reads, rec_keys, rec_values, log_decay, learn_rate, group_gain):
    read_vals = reads.astype(jnp.float32).reshape(SEQUENCE_LENGTH, RECURRENT_HEADS, HEAD)
    key_vals = rec_keys.astype(jnp.float32).reshape(SEQUENCE_LENGTH, RECURRENT_HEADS, HEAD)
    value_vals = rec_values.astype(jnp.float32).reshape(SEQUENCE_LENGTH, RECURRENT_HEADS, HEAD)
    unit_key = key_vals * lax.rsqrt(lax.optimization_barrier(jnp.sum(key_vals * key_vals, axis=-1, keepdims=True)) + KEY_EPS)
    removal = -unit_key
    writing = unit_key * learn_rate.reshape(RECURRENT_HEADS, HEAD)
    decay_vals = jnp.exp(log_decay.reshape(SEQUENCE_LENGTH, RECURRENT_HEADS, HEAD))

    def token_step(head_state, inputs):
        read_now, decay_now, key_now, current_value, removal_now, writing_now = inputs
        along_vec = jnp.einsum('hij,hj->hi', head_state, removal_now, precision=EXACT_PRECISION)
        head_state = head_state * decay_now[:, None, :] + along_vec[:, :, None] * writing_now[:, None, :] + current_value[:, :, None] * key_now[:, None, :]
        return (head_state, jnp.einsum('hij,hj->hi', head_state, read_now, precision=EXACT_PRECISION))
    zero_state = jnp.zeros((RECURRENT_HEADS, HEAD, HEAD), jnp.float32)
    _, read_out = lax.scan(token_step, zero_state, (read_vals, decay_vals, key_vals, value_vals, removal, writing))
    mean_val = lax.optimization_barrier(jnp.mean(read_out, axis=-1, keepdims=True))
    centered = read_out - mean_val
    variance = lax.optimization_barrier(jnp.mean(centered * centered, axis=-1, keepdims=True))
    normed = (centered * lax.rsqrt(variance + GROUP_EPS)).reshape(SEQUENCE_LENGTH, REC_WIDTH) * group_gain
    return normed.astype(jnp.bfloat16)

def reference(tokens, norm_gain, query_w, key_w, value_w, recept_w, rec_key_w, rec_value_w, decay_down, decay_up, decay_base, learn_rate, query_gain, key_gain, sink_logit, group_gain, out_att_w, out_rec_w):
    full_rows = tokens.astype(jnp.float32)
    mean_sq = lax.optimization_barrier(jnp.mean(full_rows * full_rows, axis=-1, keepdims=True))
    hidden = (full_rows * lax.rsqrt(mean_sq + NORM_EPS) * norm_gain).astype(jnp.bfloat16)
    query_rows = project(hidden, query_w)
    key_rows = project(hidden, key_w)
    att_values = project(hidden, value_w)
    reads = project(hidden, recept_w)
    rec_keys = project(hidden, rec_key_w)
    rec_values = project(hidden, rec_value_w)
    decay_low = jnp.tanh(jnp.dot(hidden, decay_down, preferred_element_type=jnp.float32)).astype(jnp.bfloat16)
    decay_rate = jnp.dot(decay_low, decay_up, preferred_element_type=jnp.float32) + jnp.repeat(decay_base.T, HEAD, axis=1)
    log_decay = -jnp.exp(decay_rate)
    query_n = head_rms(query_rows, query_gain, ATT_HEADS)
    key_n = head_rms(key_rows, key_gain, KV_HEADS)
    att_mix, row_lse = attention(query_n, key_n, att_values, sink_logit)
    rec_mix = recurrence(reads, rec_keys, rec_values, log_decay, learn_rate, group_gain)
    groups = N_FS * N_TP
    att_span = ATT_WIDTH // groups
    rec_span = REC_WIDTH // groups
    acc_total = jnp.zeros((SEQUENCE_LENGTH, D), jnp.float32)
    for group_index in range(groups):
        att_lo = group_index * att_span
        rec_lo = group_index * rec_span
        group_partial = jnp.dot(att_mix[:, att_lo:att_lo + att_span], out_att_w[att_lo:att_lo + att_span], preferred_element_type=jnp.float32) + jnp.dot(rec_mix[:, rec_lo:rec_lo + rec_span], out_rec_w[rec_lo:rec_lo + rec_span], preferred_element_type=jnp.float32)
        acc_total = acc_total + lax.optimization_barrier(group_partial.astype(jnp.bfloat16)).astype(jnp.float32)
    return (acc_total.astype(jnp.bfloat16), row_lse)
```

```python
import functools
import math

import jax
import jax.numpy as jnp
from jax import lax
from jax.experimental import pallas as pl
from jax.experimental.pallas import tpu as pltpu
from jax.sharding import PartitionSpec as P

HEAD = 64
WINDOW = 128
BLOCK = 32


NORM_EPS = 1e-06
KEY_EPS = 1e-06
GROUP_EPS = 0.00064
EXACT_PRECISION = lax.Precision.HIGHEST


def passed_along(array, axis, by):
    devices = lax.axis_size(axis)
    pairs = [(i, i + by) for i in range(devices) if 0 <= i + by < devices]
    return lax.ppermute(array, axis, pairs)


def prefix(array, axis, combine, identity):
    devices, place = (lax.axis_size(axis), lax.axis_index(axis))
    everything = lax.all_gather(array.astype(jnp.bfloat16), axis)
    start = jnp.broadcast_to(jnp.asarray(identity, array.dtype), array.shape)

    def turn(k, before):
        reached = k < place
        new = combine(before, everything[k].astype(array.dtype))
        return jnp.where(reached, new, before)

    return lax.fori_loop(0, devices, turn, start)


def head_rms(values, gain_vec, num_heads):
    shaped = values.astype(jnp.float32).reshape(values.shape[0], num_heads, HEAD)
    mean_sq = jnp.mean(shaped * shaped, axis=-1, keepdims=True)
    return (shaped * lax.rsqrt(mean_sq + NORM_EPS) * gain_vec).astype(jnp.bfloat16)


def attend(query_rows, key_rows, value_rows, query_gain, key_gain, sink_logit):
    num_rows = query_rows.shape[0]
    num_heads = query_rows.shape[1] // HEAD
    kv_heads = key_rows.shape[1] // HEAD
    group_size = num_heads // kv_heads
    blocks = num_rows // WINDOW
    query_n = head_rms(query_rows, query_gain, num_heads).reshape(
        blocks, WINDOW, kv_heads, group_size, HEAD
    )
    key_n = head_rms(key_rows, key_gain, kv_heads).reshape(num_rows, kv_heads * HEAD)
    paired = jnp.concatenate([key_n, value_rows], axis=1)
    before = passed_along(paired[num_rows - WINDOW :], "sp", 1)
    current = paired.reshape(blocks, WINDOW, 2 * kv_heads * HEAD)
    previous = jnp.concatenate([before[None], current[:-1]], axis=0)
    key_band = jnp.concatenate([previous, current], axis=1).reshape(
        blocks, 2 * WINDOW, 2, kv_heads, HEAD
    )
    scores = jnp.einsum(
        "nqkgd,nskd->nkgqs", query_n, key_band[:, :, 0], preferred_element_type=jnp.float32
    ) * (1.0 / math.sqrt(HEAD))
    offset = lax.axis_index("sp") * num_rows
    lag_table = (
        lax.broadcasted_iota(jnp.int32, (WINDOW, 2 * WINDOW), 0)
        + WINDOW
        - lax.broadcasted_iota(jnp.int32, (WINDOW, 2 * WINDOW), 1)
    )
    key_place = (
        offset
        + (lax.broadcasted_iota(jnp.int32, (blocks, 2 * WINDOW), 0) - 1) * WINDOW
        + lax.broadcasted_iota(jnp.int32, (blocks, 2 * WINDOW), 1)
    )
    allowed = ((lag_table >= 0) & (lag_table < WINDOW))[None, :, :] & (key_place >= 0)[:, None, :]
    allowed = allowed[:, None, None]
    sink_cols = sink_logit.reshape(kv_heads, group_size)[None, :, :, None, None]
    masked = jnp.where(allowed, scores, -jnp.inf)
    row_top = jnp.maximum(jnp.max(masked, axis=-1, keepdims=True), sink_cols)
    weight = jnp.where(allowed, jnp.exp(masked - row_top), 0.0)
    row_total = jnp.sum(weight, axis=-1, keepdims=True) + jnp.exp(sink_cols - row_top)
    row_lse = (
        (row_top + jnp.log(row_total))[..., 0].transpose(1, 2, 0, 3).reshape(num_heads, num_rows)
    )
    att_probs = (weight / row_total).astype(jnp.bfloat16)
    mixed_heads = jnp.einsum(
        "nkgqs,nskd->nqkgd", att_probs, key_band[:, :, 1], preferred_element_type=jnp.float32
    )
    return (mixed_heads.reshape(num_rows, num_heads * HEAD).astype(jnp.bfloat16), row_lse)


def unit_inverse(lower_mat):
    mat_size = lower_mat.shape[-1]
    result = jnp.eye(mat_size, dtype=jnp.float32) + lower_mat
    power_mat = lower_mat
    for section_index in range(mat_size.bit_length() - 2):
        power_mat = jnp.einsum("hij,hjk->hik", power_mat, power_mat, precision=EXACT_PRECISION)
        result = result + jnp.einsum("hij,hjk->hik", result, power_mat, precision=EXACT_PRECISION)
    return result


def pair_table(left_vals, right_vals, allowed):
    return jnp.where(
        allowed, jnp.einsum("hid,hjd->hij", left_vals, right_vals, precision=EXACT_PRECISION), 0.0
    )


def recur(reads, rec_keys, rec_values, log_decay, learn_rate, group_gain):
    num_rows = reads.shape[0]
    num_heads = reads.shape[1] // HEAD
    blocks = num_rows // BLOCK

    def by_block(values):
        return (
            values.astype(jnp.float32).reshape(blocks, BLOCK, num_heads, HEAD).transpose(0, 2, 1, 3)
        )

    read_vals = by_block(reads)
    key_vals = by_block(rec_keys)
    value_vals = by_block(rec_values)
    decay_vals = by_block(log_decay)
    unit_key = key_vals * lax.rsqrt(jnp.sum(key_vals * key_vals, axis=-1, keepdims=True) + KEY_EPS)
    removal = -unit_key
    writing = unit_key * learn_rate.reshape(num_heads, HEAD)[None, :, None, :]
    stacked = jnp.concatenate([jnp.zeros_like(value_vals), value_vals], axis=-1)
    unit_matrix = jnp.broadcast_to(jnp.eye(HEAD, dtype=jnp.float32), (num_heads, HEAD, HEAD))
    start_pair = jnp.concatenate(
        [unit_matrix, jnp.zeros((num_heads, HEAD, HEAD), jnp.float32)], axis=1
    )
    row_iota = lax.broadcasted_iota(jnp.int32, (BLOCK, BLOCK), 0)
    col_iota = lax.broadcasted_iota(jnp.int32, (BLOCK, BLOCK), 1)
    strict = (row_iota > col_iota)[None]
    inclusive = (row_iota >= col_iota)[None]

    def block_step(state_per_block, inputs):
        read_now, key_now, removal_now, writing_now, decay_now, current_value = inputs
        cum_decay = jnp.cumsum(decay_now, axis=1)
        decay_matrix_a = removal_now * jnp.exp(cum_decay - decay_now)
        decay_matrix_b = writing_now * jnp.exp(-cum_decay)
        stacked_key_matrix = key_now * jnp.exp(-cum_decay)
        stacked_receptance = read_now * jnp.exp(cum_decay)
        m_ab = pair_table(decay_matrix_a, decay_matrix_b, strict)
        m_ak = pair_table(decay_matrix_a, stacked_key_matrix, strict)
        m_rb = pair_table(stacked_receptance, decay_matrix_b, inclusive)
        m_rk = pair_table(stacked_receptance, stacked_key_matrix, inclusive)
        right_operand = jnp.einsum(
            "bvq,bzq->bvz", decay_matrix_a, state_per_block, precision=EXACT_PRECISION
        ) + jnp.einsum("hij,hjm->him", m_ak, current_value, precision=EXACT_PRECISION)
        delta_updates = jnp.einsum(
            "hij,hjm->him", unit_inverse(m_ab), right_operand, precision=EXACT_PRECISION
        )
        block_out = (
            jnp.einsum(
                "bvq,bzq->bvz", stacked_receptance, state_per_block, precision=EXACT_PRECISION
            )
            + jnp.einsum("hij,hjm->him", m_rb, delta_updates, precision=EXACT_PRECISION)
            + jnp.einsum("hij,hjm->him", m_rk, current_value, precision=EXACT_PRECISION)
        )
        grown_state = (
            state_per_block
            + jnp.einsum("sao,sac->soc", delta_updates, decay_matrix_b, precision=EXACT_PRECISION)
            + jnp.einsum(
                "sao,sac->soc", current_value, stacked_key_matrix, precision=EXACT_PRECISION
            )
        )
        return (grown_state * jnp.exp(cum_decay[:, -1])[:, None, :], block_out)

    final_state, block_outs = lax.scan(
        block_step, start_pair, (read_vals, key_vals, removal, writing, decay_vals, stacked)
    )

    def chain(earlier, later_pair):
        moved_state = jnp.einsum(
            "hmk,hkj->hmj", earlier, later_pair[:, :HEAD], precision=EXACT_PRECISION
        )
        return moved_state + jnp.concatenate(
            [jnp.zeros_like(later_pair[:, HEAD:]), later_pair[:, HEAD:]], axis=1
        )

    carried = prefix(final_state, "sp", chain, start_pair)
    incoming = carried[:, HEAD:]
    result = block_outs[..., HEAD:] + jnp.einsum(
        "nhlm,hvm->nhlv", block_outs[..., :HEAD], incoming, precision=EXACT_PRECISION
    )
    mean_val = jnp.mean(result, axis=-1, keepdims=True)
    centered = result - mean_val
    variance = jnp.mean(centered * centered, axis=-1, keepdims=True)
    normed = (
        (centered * lax.rsqrt(variance + GROUP_EPS))
        .transpose(0, 2, 1, 3)
        .reshape(num_rows, num_heads * HEAD)
    )
    return (normed * group_gain).astype(jnp.bfloat16)


def per_device(
    tokens,
    norm_gain,
    query_w,
    key_w,
    value_w,
    recept_w,
    rec_key_w,
    rec_value_w,
    decay_down,
    decay_up,
    decay_base,
    learn_rate,
    query_gain,
    key_gain,
    sink_logit,
    group_gain,
    out_att_w,
    out_rec_w,
):
    groups = lax.axis_size(("fs", "tp"))
    own_width = tokens.shape[1]
    own_values = tokens.astype(jnp.float32)
    squares = lax.psum(jnp.sum(own_values * own_values, axis=1), ("fs", "tp"))
    gain_part = lax.dynamic_slice_in_dim(
        norm_gain, lax.axis_index(("fs", "tp")) * own_width, own_width, 0
    )
    scaled = own_values * lax.rsqrt(squares / (own_width * groups) + NORM_EPS)[:, None] * gain_part
    outgoing = scaled.astype(jnp.bfloat16)
    gathered = lax.all_gather(outgoing, ("fs", "tp"), axis=1, tiled=True)

    def rounded(sums):
        return lax.optimization_barrier(
            tuple((acc_total.astype(jnp.bfloat16) for acc_total in sums))
        )

    rec_span = recept_w.shape[1]
    decay_cols = lax.dynamic_slice_in_dim(
        decay_up, lax.axis_index(("fs", "tp")) * rec_span, rec_span, 1
    )
    decay_low = jnp.tanh(jnp.dot(gathered, decay_down, preferred_element_type=jnp.float32)).astype(
        jnp.bfloat16
    )
    decay_rate = jnp.dot(decay_low, decay_cols, preferred_element_type=jnp.float32) + jnp.repeat(
        decay_base.T, HEAD, axis=1
    )
    log_decay = -jnp.exp(decay_rate)
    pieces = (
        lax.all_gather(query_w, "sp", axis=0, tiled=True),
        lax.all_gather(key_w, "sp", axis=0, tiled=True),
        lax.all_gather(value_w, "sp", axis=0, tiled=True),
        lax.all_gather(recept_w, "sp", axis=0, tiled=True),
        lax.all_gather(rec_key_w, "sp", axis=0, tiled=True),
        lax.all_gather(rec_value_w, "sp", axis=0, tiled=True),
    )
    all_sums = tuple(
        (
            jnp.dot(gathered, weight_piece, preferred_element_type=jnp.float32)
            for weight_piece in pieces
        )
    )
    att_inputs = rounded(all_sums[:3])
    att_mix, row_lse = attend(
        att_inputs[0], att_inputs[1], att_inputs[2], query_gain, key_gain, sink_logit
    )
    rec_sums = all_sums[3:]
    rec_inputs = rounded(rec_sums)
    rec_mix = recur(rec_inputs[0], rec_inputs[1], rec_inputs[2], log_decay, learn_rate, group_gain)
    att_full, rec_full = (
        lax.all_gather(out_att_w, "sp", axis=1, tiled=True),
        lax.all_gather(out_rec_w, "sp", axis=1, tiled=True),
    )
    mixed_out = lax.psum_scatter(
        (
            jnp.dot(att_mix, att_full, preferred_element_type=jnp.float32)
            + jnp.dot(rec_mix, rec_full, preferred_element_type=jnp.float32)
        ).astype(jnp.bfloat16),
        ("fs", "tp"),
        scatter_dimension=0,
        tiled=True,
    )
    return (mixed_out, row_lse)


def general(mesh):
    in_specs = (
        P("sp", ("fs", "tp")),
        P(),
        P("sp", ("fs", "tp")),
        P("sp", ("fs", "tp")),
        P("sp", ("fs", "tp")),
        P("sp", ("fs", "tp")),
        P("sp", ("fs", "tp")),
        P("sp", ("fs", "tp")),
        P(),
        P(),
        P(("fs", "tp"), "sp"),
        P(("fs", "tp")),
        P(),
        P(),
        P(("fs", "tp")),
        P(("fs", "tp")),
        P(("fs", "tp"), "sp"),
        P(("fs", "tp"), "sp"),
    )
    out_specs = (P(("sp", "fs", "tp"), None), P(("fs", "tp"), "sp"))
    return jax.shard_map(
        per_device, mesh=mesh, in_specs=in_specs, out_specs=out_specs, check_vma=False
    )


LANES = 128
CHUNK = 64
MESH = pl.DeviceIdType.MESH


def dot(a, b):
    return jnp.dot(a, b, preferred_element_type=jnp.float32)


def dot_t(a, b, dims):
    return lax.dot_general(a, b, (dims, ((), ())), preferred_element_type=jnp.float32)


def halves(values):
    high = values.astype(jnp.bfloat16)
    return high, (values - high.astype(jnp.float32)).astype(jnp.bfloat16)


def exact(a, b, dims=((1,), (0,))):
    a_hi, a_lo = halves(a)
    b_hi, b_lo = halves(b)
    return dot_t(a_hi, b_hi, dims) + (dot_t(a_hi, b_lo, dims) + dot_t(a_lo, b_hi, dims))


def layer_kernel(n_sp, n_fs, n_tp, *refs):
    (tok, gain, recept_w, rec_key_w, rec_value_w, query_w, kv_w, out_att, out_rec) = refs[:9]
    (down, up, base, rate, q_gain, k_gain, sink, g_gain, out, lse_out) = refs[9:19]
    w_bufs = refs[19:26]
    (tok_buf, hid, halo_out, halo_in, state_out, state_in, part, part_in) = refs[26:34]
    (ward_out, ward_low, got, got_low) = refs[34:38]
    (ring_send, ring_recv, chip_send, chip_recv, core_send, core_recv, ward_send, ward_recv,
     one_send, one_recv, st_send, st_recv, red_send, red_recv) = refs[38:]
    weights = (recept_w, rec_key_w, rec_value_w, query_w, kv_w, out_att, out_rec)
    groups = n_fs * n_tp
    place = lax.axis_index("sp")
    own = lax.axis_index("fs") * n_tp + lax.axis_index("tp")
    rows = tok.shape[0]

    def peer(step):
        other = lax.rem(own + step, groups)
        return {"fs": lax.div(other, n_tp), "tp": lax.rem(other, n_tp)}

    barrier = pltpu.get_barrier_semaphore()
    for step in range(1, groups):
        pl.semaphore_signal(barrier, inc=1, device_id=peer(step), device_id_type=MESH)
    for step in range(1, n_sp):
        pl.semaphore_signal(
            barrier, inc=1, device_id={"sp": lax.rem(place + step, n_sp)}, device_id_type=MESH
        )
    pl.semaphore_wait(barrier, groups - 1 + n_sp - 1)

    def hop(item, way, step):
        sign = 1 if way == 0 else -1
        src = weights[item] if step == 0 else w_bufs[item].at[lax.rem(place - sign * step + n_sp, n_sp)]
        return pltpu.make_async_remote_copy(
            src_ref=src,
            dst_ref=w_bufs[item].at[lax.rem(place - sign * step + n_sp, n_sp)],
            send_sem=ring_send.at[item, way, step],
            recv_sem=ring_recv.at[item, way, step],
            device_id={"sp": lax.rem(place + sign + n_sp, n_sp)},
            device_id_type=MESH,
        )

    def inner(at):
        return (at >= 1) & (at <= n_sp - 2)

    inside = inner(place)
    outside = ~inside
    helps = inside & ((place == 1) | (place == n_sp - 2))
    partner = jnp.where(
        place == 0, 1, jnp.where(place == n_sp - 1, n_sp - 2, jnp.where(place == 1, 0, n_sp - 1))
    )
    inputs = 5

    def sends(item, way, step):
        if way == 0:
            base_case, to = (place >= step) & (place + 1 < n_sp), place + 1
        else:
            base_case, to = (place + step < n_sp) & (place >= 1), place - 1
        return base_case & inner(to) if item < inputs else base_case

    def takes(item, way, step):
        base_case = place >= step + 1 if way == 0 else place + step + 1 < n_sp
        return base_case & inside if item < inputs else base_case

    def start(items, step, to_inner):
        for item in items:
            for way in (0, 1):
                to = inner(place + (1 if way == 0 else -1))

                @pl.when(sends(item, way, step) & (to if to_inner else ~to))
                def _():
                    hop(item, way, step).start()

    def sent(item, step):
        for way in (0, 1):

            @pl.when(sends(item, way, step))
            def _():
                hop(item, way, step).wait_send()

    def relay(items, step, from_inner):
        for item in items:
            for way in (0, 1):
                origin = inner(place - (1 if way == 0 else -1))
                mine = inside & (origin if from_inner else ~origin)

                @pl.when(takes(item, way, step) & mine)
                def _():
                    hop(item, way, step).wait_recv()

                if step + 1 < n_sp - 1:

                    @pl.when(sends(item, way, step + 1) & mine)
                    def _():
                        hop(item, way, step + 1).start()

    rec_items, att_items, out_items = (0, 1, 2), (3, 4), (5, 6)

    def ward_tok():
        return pltpu.make_async_remote_copy(
            src_ref=tok, dst_ref=tok_buf.at[1, own], send_sem=ward_send.at[0],
            recv_sem=ward_recv.at[0], device_id={"sp": partner}, device_id_type=MESH,
        )

    fs_at, tp_at = lax.axis_index("fs"), lax.axis_index("tp")

    def chip_copy(which, step):
        return pltpu.make_async_remote_copy(
            src_ref=tok if which == 0 else tok_buf.at[1, own], dst_ref=tok_buf.at[which, own],
            send_sem=chip_send.at[which, step - 1], recv_sem=chip_recv.at[which, step - 1],
            device_id={"fs": lax.rem(fs_at + step, n_fs)}, device_id_type=MESH,
        )

    def core_copy(which, step, turn):
        slot = lax.rem(fs_at - step + n_fs, n_fs) * n_tp + tp_at
        return pltpu.make_async_remote_copy(
            src_ref=tok if which == 0 and step == 0 else tok_buf.at[which, slot],
            dst_ref=tok_buf.at[which, slot],
            send_sem=core_send.at[which, step, turn - 1], recv_sem=core_recv.at[which, step, turn - 1],
            device_id={"tp": lax.rem(tp_at + turn, n_tp)}, device_id_type=MESH,
        )

    def to_chips(which):
        for step in range(1, n_fs):
            chip_copy(which, step).start()
        for turn in range(1, n_tp):
            core_copy(which, 0, turn).start()

    def to_cores(which):
        for step in range(1, n_fs):
            chip_copy(which, step).wait_recv()
            for turn in range(1, n_tp):
                core_copy(which, step, turn).start()

    def all_tokens(which):
        for step in range(n_fs):
            for turn in range(1, n_tp):
                core_copy(which, step, turn).wait_recv()

    width = tok.shape[1]

    def input_norm(which):
        squares = jnp.zeros((rows, 1), jnp.float32)
        for group in range(groups):
            values = tok_buf[which, group].astype(jnp.float32)
            squares = squares + jnp.sum(values * values, axis=1, keepdims=True)
        inv_rms = lax.rsqrt(squares / (width * groups) + NORM_EPS)
        for group in range(groups):
            cut = slice(group * width, (group + 1) * width)
            hid[which, :, cut] = (
                tok_buf[which, group].astype(jnp.float32) * inv_rms * gain[:, cut]
            ).astype(jnp.bfloat16)

    def project(which, item):
        buf = w_bufs[item]
        flat = buf[...].reshape(buf.shape[0] * buf.shape[1], buf.shape[2])
        return dot(hid[which], flat).astype(jnp.bfloat16)

    def low_rank(which):
        return jnp.tanh(dot(hid[which], down[...])).astype(jnp.bfloat16)

    def ward_copy(item):
        source, target = (ward_low, got_low) if item == inputs else (ward_out.at[item], got.at[item])
        return pltpu.make_async_remote_copy(
            src_ref=source, dst_ref=target, send_sem=ward_send.at[1 + item],
            recv_sem=ward_recv.at[1 + item], device_id={"sp": partner}, device_id_type=MESH,
        )

    @pl.when(outside)
    def _():
        ward_tok().start()

    @pl.when(inside)
    def _():
        to_chips(0)

    start(rec_items, 0, True)
    start(out_items, 0, False)

    @pl.when(outside)
    def _():
        start(att_items, 0, True)
        start(out_items, 0, True)

    tok_buf[0, own] = tok[...]
    for item in range(len(weights)):
        w_bufs[item][place] = weights[item][...]

    @pl.when(place == 0)
    def _():
        halo_in[...] = jnp.zeros_like(halo_in)

    @pl.when(helps)
    def _():
        ward_tok().wait_recv()
        to_chips(1)

    @pl.when(inside)
    def _():
        to_cores(0)

    relay(rec_items[:2], 0, False)

    @pl.when(inside)
    def _():
        all_tokens(0)
        input_norm(0)

    relay(rec_items[2:], 0, False)
    relay(rec_items, 0, True)

    @pl.when(inside)
    def _():
        start(att_items, 0, True)

    @pl.when(helps)
    def _():
        to_cores(1)
        all_tokens(1)
        input_norm(1)

    relay(att_items, 0, False)

    @pl.when(inside)
    def _():
        start(out_items, 0, True)

    for step in range(1, n_sp - 2):
        relay(rec_items, step, True)

    @pl.when(helps)
    def _():
        for item in rec_items:
            ward_out[item] = project(1, item)
        ward_low[...] = low_rank(1)

    @pl.when(inside)
    def _():
        got_low[...] = low_rank(0)

    @pl.when(helps)
    def _():
        for item in rec_items + (inputs,):
            ward_copy(item).start()

    @pl.when(inside)
    def _():
        for item in rec_items:
            got[item] = project(0, item)

    @pl.when(outside)
    def _():
        for item in rec_items + (inputs,):
            ward_copy(item).wait_recv()

    span = up.shape[1]
    log_decay = -jnp.exp(dot(got_low[...], up[...]) + base[...])
    reads = got[0].astype(jnp.float32)
    keys = got[1].astype(jnp.float32)
    vals = got[2].astype(jnp.float32)

    chunks = rows // CHUNK
    row_at = lax.broadcasted_iota(jnp.int32, (rows, rows), 0)
    col_at = lax.broadcasted_iota(jnp.int32, (rows, rows), 1)
    same = lax.div(row_at, CHUNK) == lax.div(col_at, CHUNK)
    inclusive = same & (row_at >= col_at)
    strict = same & (row_at > col_at)
    ones = jnp.where(inclusive, 1.0, 0.0).astype(jnp.bfloat16)
    ld_hi, ld_lo = halves(log_decay)
    ld_rest = (log_decay - ld_hi.astype(jnp.float32) - ld_lo.astype(jnp.float32)).astype(jnp.bfloat16)
    cum = dot(ones, ld_hi) + (dot(ones, ld_lo) + dot(ones, ld_rest))
    cum_c = cum.reshape(chunks, CHUNK, span)
    middle = cum_c[:, CHUNK // 2 - 1 : CHUNK // 2, :]
    last = cum_c[:, CHUNK - 1 : CHUNK, :]
    rel = (cum_c - middle).reshape(rows, span)
    to_end = jnp.exp(last - cum_c).reshape(rows, span)
    eye = jnp.where(
        lax.broadcasted_iota(jnp.int32, (HEAD, HEAD), 0) == lax.broadcasted_iota(jnp.int32, (HEAD, HEAD), 1),
        1.0, 0.0,
    )
    big_eye = jnp.where(row_at == col_at, 1.0, 0.0)
    zeros = jnp.zeros((HEAD, HEAD), jnp.float32)
    rec_heads = span // HEAD
    from_start, own_part = [], []
    for head in range(rec_heads):
        at = slice(head * HEAD, (head + 1) * HEAD)
        k, v, r = keys[:, at], vals[:, at], reads[:, at]
        unit = k * lax.rsqrt(jnp.sum(k * k, axis=1, keepdims=True) + KEY_EPS)
        write = unit * rate[:, at]
        before = cum[:, at] - log_decay[:, at]
        up_rel, down_rel = jnp.exp(rel[:, at]), jnp.exp(-rel[:, at])
        left = jnp.concatenate([-unit * jnp.exp(rel[:, at] - log_decay[:, at]), r * up_rel], axis=0)
        right = jnp.concatenate([write * down_rel, k * down_rel], axis=0)
        table = exact(left, right, ((1,), (1,)))
        m_ab = jnp.where(strict, table[:rows, :rows], 0.0)
        m_ak = jnp.where(strict, table[:rows, rows:], 0.0)
        m_rb = jnp.where(inclusive, table[rows:, :rows], 0.0)
        m_rk = jnp.where(inclusive, table[rows:, rows:], 0.0)
        inverse, power = big_eye + m_ab, m_ab
        for _ in range(CHUNK.bit_length() - 2):
            power = exact(power, power)
            inverse = inverse + exact(inverse, power)
        pu = exact(inverse, jnp.concatenate([-unit * jnp.exp(before), exact(m_ak, v)], axis=1))
        mixed_pu = exact(m_rb, pu)
        given = r * jnp.exp(cum[:, at]) + mixed_pu[:, :HEAD]
        offset = mixed_pu[:, HEAD:] + exact(m_rk, v)
        b_end, k_end = write * to_end[:, at], k * to_end[:, at]
        pair = jnp.concatenate([eye, zeros], axis=1)
        reach = []
        for chunk in range(chunks):
            cut = slice(chunk * CHUNK, (chunk + 1) * CHUNK)
            reach.append(exact(given[cut], pair))
            step_map = exact(b_end[cut], pu[cut], ((0,), (0,)))
            turn = step_map[:, :HEAD] + eye * jnp.exp(last[chunk][:, at])
            grown = step_map[:, HEAD:] + exact(k_end[cut], v[cut], ((0,), (0,)))
            pair = exact(turn, pair) + jnp.concatenate([zeros, grown], axis=1)
        reach = jnp.concatenate(reach, axis=0)
        from_start.append(reach[:, :HEAD])
        own_part.append(reach[:, HEAD:] + offset)
        state_out[head] = pair.astype(jnp.bfloat16)
        if head == 0:
            relay(out_items, 0, False)

    def state_copy(step):
        return pltpu.make_async_remote_copy(
            src_ref=state_out, dst_ref=state_in.at[place], send_sem=st_send.at[step - 1],
            recv_sem=st_recv.at[step - 1], device_id={"sp": lax.rem(place + step, n_sp)},
            device_id_type=MESH,
        )

    for step in range(n_sp - 2):
        relay(att_items, step, True)
    for step in range(1, n_sp):
        @pl.when(place + step < n_sp)
        def _():
            state_copy(step).start()

    @pl.when(helps)
    def _():
        for item in att_items:
            ward_out[item] = project(1, item)

    @pl.when(inside)
    def _():
        for item in att_items:
            got[item] = project(0, item)

    @pl.when(helps)
    def _():
        for item in att_items:
            ward_copy(item).start()

    relay(out_items, 0, True)

    @pl.when(outside)
    def _():
        for item in att_items:
            ward_copy(item).wait_recv()

    q_all = got[3].astype(jnp.float32)
    kv_all = got[4].astype(jnp.float32)
    kv_heads = kv_all.shape[1] // (2 * HEAD)
    q_heads = q_all.shape[1] // HEAD
    share = q_heads // kv_heads

    def normed(values, gain_ref):
        mean_sq = jnp.mean(values * values, axis=1, keepdims=True)
        return (values * lax.rsqrt(mean_sq + NORM_EPS) * gain_ref[...]).astype(jnp.bfloat16)

    key_n = [normed(kv_all[:, h * HEAD : (h + 1) * HEAD], k_gain) for h in range(kv_heads)]
    value_n = [
        kv_all[:, (kv_heads + h) * HEAD : (kv_heads + h + 1) * HEAD].astype(jnp.bfloat16)
        for h in range(kv_heads)
    ]
    halo_out[...] = jnp.concatenate([x[rows - WINDOW :] for x in key_n + value_n], axis=1)
    query_n = [normed(q_all[:, h * HEAD : (h + 1) * HEAD], q_gain) for h in range(q_heads)]

    def halo_copy():
        return pltpu.make_async_remote_copy(
            src_ref=halo_out, dst_ref=halo_in, send_sem=one_send.at[0], recv_sem=one_recv.at[0],
            device_id={"sp": lax.rem(place + 1, n_sp)}, device_id_type=MESH,
        )

    @pl.when(place + 1 < n_sp)
    def _():
        halo_copy().start()

    blocks = rows // WINDOW
    lag = (
        lax.broadcasted_iota(jnp.int32, (WINDOW, 2 * WINDOW), 0)
        + WINDOW
        - lax.broadcasted_iota(jnp.int32, (WINDOW, 2 * WINDOW), 1)
    )
    key_col = lax.broadcasted_iota(jnp.int32, (WINDOW, 2 * WINDOW), 1)
    mixes = [[None] * q_heads for _ in range(blocks)]

    def attend_block(block, band_keys, band_values):
        allowed = (lag >= 0) & (lag < WINDOW)
        if block == 0:
            allowed = allowed & (key_col + (place * blocks - 1) * WINDOW >= 0)
        cut = slice(block * WINDOW, (block + 1) * WINDOW)
        for h in range(q_heads):
            top_sink = sink[0, h]
            scores = dot_t(query_n[h][cut], band_keys[h // share], ((1,), (1,))) * (1.0 / math.sqrt(HEAD))
            masked = jnp.where(allowed, scores, -jnp.inf)
            top = jnp.maximum(jnp.max(masked, axis=1, keepdims=True), top_sink)
            weight = jnp.where(allowed, jnp.exp(masked - top), 0.0)
            total = jnp.sum(weight, axis=1, keepdims=True) + jnp.exp(top_sink - top)
            spread = jnp.broadcast_to(top + jnp.log(total), (WINDOW, LANES)).T
            lse_out[h : h + 1, cut] = spread[0:1]
            probs = (weight / total).astype(jnp.bfloat16)
            mixes[block][h] = dot(probs, band_values[h // share]).astype(jnp.bfloat16)

    for block in range(1, blocks):
        band = slice((block - 1) * WINDOW, (block + 1) * WINDOW)
        attend_block(block, [x[band] for x in key_n], [x[band] for x in value_n])

    @pl.when(place >= 1)
    def _():
        halo_copy().wait_recv()

    halo = halo_in[...]
    before_k = [halo[:, h * HEAD : (h + 1) * HEAD] for h in range(kv_heads)]
    before_v = [halo[:, (kv_heads + h) * HEAD : (kv_heads + h + 1) * HEAD] for h in range(kv_heads)]
    attend_block(
        0,
        [jnp.concatenate([b, x[:WINDOW]], axis=0) for b, x in zip(before_k, key_n)],
        [jnp.concatenate([b, x[:WINDOW]], axis=0) for b, x in zip(before_v, value_n)],
    )
    att_mix = jnp.concatenate([jnp.concatenate(line, axis=1) for line in mixes], axis=0)
    for step in range(1, n_sp - 2):
        relay(out_items, step, True)

    @pl.when(outside)
    def _():
        for item in out_items:
            for step in range(n_sp - 1):
                for way in (0, 1):

                    @pl.when(takes(item, way, step))
                    def _():
                        hop(item, way, step).wait_recv()

    for step in range(1, n_sp):
        @pl.when(place >= step)
        def _():
            state_copy(step).wait_recv()
    rec_parts = []
    for head in range(rec_heads):
        state = zeros
        for k in range(n_sp - 1):
            pair = state_in[k, head].astype(jnp.float32)
            moved = exact(pair[:, :HEAD], state) + pair[:, HEAD:]
            state = jnp.where(place > k, moved, state)
        result = own_part[head] + exact(from_start[head], state)
        mean_val = jnp.mean(result, axis=1, keepdims=True)
        centered = result - mean_val
        variance = jnp.mean(centered * centered, axis=1, keepdims=True)
        at = slice(head * HEAD, (head + 1) * HEAD)
        rec_parts.append((centered * lax.rsqrt(variance + GROUP_EPS) * g_gain[:, at]).astype(jnp.bfloat16))
    rec_mix = jnp.concatenate(rec_parts, axis=1)

    cols = out_att.shape[1]
    few = rows // groups
    for k in range(n_sp):
        block = (dot(att_mix, w_bufs[5][k]) + dot(rec_mix, w_bufs[6][k])).astype(jnp.bfloat16)
        part[:, :, k * cols : (k + 1) * cols] = block.reshape(groups, few, cols)

    def red_copy(step):
        return pltpu.make_async_remote_copy(
            src_ref=part.at[lax.rem(own + step, groups)], dst_ref=part_in.at[step - 1],
            send_sem=red_send.at[step - 1], recv_sem=red_recv.at[step - 1],
            device_id=peer(step), device_id_type=MESH,
        )

    for step in range(1, groups):
        red_copy(step).start()
    @pl.when(outside)
    def _():
        ward_tok().wait_send()

    def tokens_sent(which):
        for step in range(1, n_fs):
            chip_copy(which, step).wait_send()
        for step in range(n_fs):
            for turn in range(1, n_tp):
                core_copy(which, step, turn).wait_send()

    @pl.when(inside)
    def _():
        tokens_sent(0)

    @pl.when(helps)
    def _():
        tokens_sent(1)
        for item in range(inputs + 1):
            ward_copy(item).wait_send()

    for item in range(len(weights)):
        for step in range(n_sp - 1):
            sent(item, step)
    for step in range(1, n_sp):
        @pl.when(place + step < n_sp)
        def _():
            state_copy(step).wait_send()

    @pl.when(place + 1 < n_sp)
    def _():
        halo_copy().wait_send()

    total = part[own].astype(jnp.float32)
    for step in range(1, groups):
        red_copy(step).wait_recv()
        total = total + part_in[step - 1].astype(jnp.float32)
    out[...] = total.astype(jnp.bfloat16)
    for step in range(1, groups):
        red_copy(step).wait_send()


def in_kernel(
    n_sp, n_fs, n_tp,
    tokens, norm_gain, query_w, key_w, value_w, recept_w, rec_key_w, rec_value_w,
    decay_down, decay_up, decay_base, learn_rate, query_gain, key_gain, sink_logit,
    group_gain, out_att_w, out_rec_w,
):
    groups = n_fs * n_tp
    rows, width = tokens.shape
    rec_span = recept_w.shape[1]
    model = width * groups
    up = lax.dynamic_slice_in_dim(decay_up, lax.axis_index(("fs", "tp")) * rec_span, rec_span, 1)
    base = jnp.repeat(decay_base.T, HEAD, axis=1)
    kv_w = jnp.concatenate([key_w, value_w], axis=1)
    weights = (recept_w, rec_key_w, rec_value_w, query_w, kv_w, out_att_w, out_rec_w)
    vmem = pl.BlockSpec(memory_space=pltpu.VMEM)
    smem = pl.BlockSpec(memory_space=pltpu.SMEM)
    bf16 = jnp.bfloat16
    heads = rec_span // HEAD
    dma = pltpu.SemaphoreType.DMA
    scratch = [pltpu.VMEM((n_sp, *w.shape), bf16) for w in weights] + [
        pltpu.VMEM((2, groups, rows, width), bf16),
        pltpu.VMEM((2, rows, model), bf16),
        pltpu.VMEM((WINDOW, kv_w.shape[1]), bf16),
        pltpu.VMEM((WINDOW, kv_w.shape[1]), bf16),
        pltpu.VMEM((heads, HEAD, 2 * HEAD), bf16),
        pltpu.VMEM((n_sp, heads, HEAD, 2 * HEAD), bf16),
        pltpu.VMEM((groups, rows // groups, model), bf16),
        pltpu.VMEM((groups - 1, rows // groups, model), bf16),
        pltpu.VMEM((5, rows, rec_span), bf16),
        pltpu.VMEM((rows, decay_down.shape[1]), bf16),
        pltpu.VMEM((5, rows, rec_span), bf16),
        pltpu.VMEM((rows, decay_down.shape[1]), bf16),
        dma((len(weights), 2, n_sp - 1)),
        dma((len(weights), 2, n_sp - 1)),
        dma((2, n_fs - 1)),
        dma((2, n_fs - 1)),
        dma((2, n_fs, n_tp - 1)),
        dma((2, n_fs, n_tp - 1)),
        dma((7,)),
        dma((7,)),
        dma((1,)),
        dma((1,)),
        dma((n_sp - 1,)),
        dma((n_sp - 1,)),
        dma((groups - 1,)),
        dma((groups - 1,)),
    ]
    return pl.pallas_call(
        functools.partial(layer_kernel, n_sp, n_fs, n_tp),
        out_shape=(
            jax.ShapeDtypeStruct((rows // groups, model), bf16),
            jax.ShapeDtypeStruct((sink_logit.shape[0], rows), jnp.float32),
        ),
        in_specs=[vmem] * 15 + [smem] + [vmem],
        out_specs=(vmem, vmem),
        scratch_shapes=scratch,
        compiler_params=pltpu.CompilerParams(
            collective_id=0, has_side_effects=True, vmem_limit_bytes=60 * 1024 * 1024
        ),
    )(
        tokens, norm_gain[None], *weights, decay_down, up, base, learn_rate[None],
        query_gain[None], key_gain[None], sink_logit[None], group_gain[None],
    )


def solution(mesh):
    n_sp, n_fs, n_tp = (mesh.shape[name] for name in ("sp", "fs", "tp"))
    plain = general(mesh)

    def layer(*arrays):
        if (arrays[-1].shape[1] // n_sp) % LANES or n_sp > LANES // 8 or n_sp < 4:
            return plain(*arrays)
        in_specs = (
            P("sp", ("fs", "tp")),
            P(),
            P("sp", ("fs", "tp")),
            P("sp", ("fs", "tp")),
            P("sp", ("fs", "tp")),
            P("sp", ("fs", "tp")),
            P("sp", ("fs", "tp")),
            P("sp", ("fs", "tp")),
            P(),
            P(),
            P(("fs", "tp"), "sp"),
            P(("fs", "tp")),
            P(),
            P(),
            P(("fs", "tp")),
            P(("fs", "tp")),
            P(("fs", "tp"), "sp"),
            P(("fs", "tp"), "sp"),
        )
        out_specs = (P(("sp", "fs", "tp"), None), P(("fs", "tp"), "sp"))
        return jax.shard_map(
            functools.partial(in_kernel, n_sp, n_fs, n_tp),
            mesh=mesh, in_specs=in_specs, out_specs=out_specs, check_vma=False,
        )(*arrays)

    return layer
```

```python
import functools
import math

import jax
import jax.numpy as jnp
from jax import lax
from jax.experimental import pallas as pl
from jax.experimental.pallas import tpu as pltpu
from jax.sharding import PartitionSpec as P

HEAD = 64
WINDOW = 128
BLOCK = 32


NORM_EPS = 1e-06
KEY_EPS = 1e-06
GROUP_EPS = 0.00064
EXACT_PRECISION = lax.Precision.HIGHEST


def passed_along(array, axis, by):
    devices = lax.axis_size(axis)
    pairs = [(i, i + by) for i in range(devices) if 0 <= i + by < devices]
    return lax.ppermute(array, axis, pairs)


def prefix(array, axis, combine, identity):
    devices, place = (lax.axis_size(axis), lax.axis_index(axis))
    everything = lax.all_gather(array.astype(jnp.bfloat16), axis)
    start = jnp.broadcast_to(jnp.asarray(identity, array.dtype), array.shape)

    def turn(k, before):
        reached = k < place
        new = combine(before, everything[k].astype(array.dtype))
        return jnp.where(reached, new, before)

    return lax.fori_loop(0, devices, turn, start)


def head_rms(values, gain_vec, num_heads):
    shaped = values.astype(jnp.float32).reshape(values.shape[0], num_heads, HEAD)
    mean_sq = jnp.mean(shaped * shaped, axis=-1, keepdims=True)
    return (shaped * lax.rsqrt(mean_sq + NORM_EPS) * gain_vec).astype(jnp.bfloat16)


def attend(query_rows, key_rows, value_rows, query_gain, key_gain, sink_logit):
    num_rows = query_rows.shape[0]
    num_heads = query_rows.shape[1] // HEAD
    kv_heads = key_rows.shape[1] // HEAD
    group_size = num_heads // kv_heads
    blocks = num_rows // WINDOW
    query_n = head_rms(query_rows, query_gain, num_heads).reshape(
        blocks, WINDOW, kv_heads, group_size, HEAD
    )
    key_n = head_rms(key_rows, key_gain, kv_heads).reshape(num_rows, kv_heads * HEAD)
    paired = jnp.concatenate([key_n, value_rows], axis=1)
    before = passed_along(paired[num_rows - WINDOW :], "sp", 1)
    current = paired.reshape(blocks, WINDOW, 2 * kv_heads * HEAD)
    previous = jnp.concatenate([before[None], current[:-1]], axis=0)
    key_band = jnp.concatenate([previous, current], axis=1).reshape(
        blocks, 2 * WINDOW, 2, kv_heads, HEAD
    )
    scores = jnp.einsum(
        "nqkgd,nskd->nkgqs", query_n, key_band[:, :, 0], preferred_element_type=jnp.float32
    ) * (1.0 / math.sqrt(HEAD))
    offset = lax.axis_index("sp") * num_rows
    lag_table = (
        lax.broadcasted_iota(jnp.int32, (WINDOW, 2 * WINDOW), 0)
        + WINDOW
        - lax.broadcasted_iota(jnp.int32, (WINDOW, 2 * WINDOW), 1)
    )
    key_place = (
        offset
        + (lax.broadcasted_iota(jnp.int32, (blocks, 2 * WINDOW), 0) - 1) * WINDOW
        + lax.broadcasted_iota(jnp.int32, (blocks, 2 * WINDOW), 1)
    )
    allowed = ((lag_table >= 0) & (lag_table < WINDOW))[None, :, :] & (key_place >= 0)[:, None, :]
    allowed = allowed[:, None, None]
    sink_cols = sink_logit.reshape(kv_heads, group_size)[None, :, :, None, None]
    masked = jnp.where(allowed, scores, -jnp.inf)
    row_top = jnp.maximum(jnp.max(masked, axis=-1, keepdims=True), sink_cols)
    weight = jnp.where(allowed, jnp.exp(masked - row_top), 0.0)
    row_total = jnp.sum(weight, axis=-1, keepdims=True) + jnp.exp(sink_cols - row_top)
    row_lse = (
        (row_top + jnp.log(row_total))[..., 0].transpose(1, 2, 0, 3).reshape(num_heads, num_rows)
    )
    att_probs = (weight / row_total).astype(jnp.bfloat16)
    mixed_heads = jnp.einsum(
        "nkgqs,nskd->nqkgd", att_probs, key_band[:, :, 1], preferred_element_type=jnp.float32
    )
    return (mixed_heads.reshape(num_rows, num_heads * HEAD).astype(jnp.bfloat16), row_lse)


def unit_inverse(lower_mat):
    mat_size = lower_mat.shape[-1]
    result = jnp.eye(mat_size, dtype=jnp.float32) + lower_mat
    power_mat = lower_mat
    for section_index in range(mat_size.bit_length() - 2):
        power_mat = jnp.einsum("hij,hjk->hik", power_mat, power_mat, precision=EXACT_PRECISION)
        result = result + jnp.einsum("hij,hjk->hik", result, power_mat, precision=EXACT_PRECISION)
    return result


def pair_table(left_vals, right_vals, allowed):
    return jnp.where(
        allowed, jnp.einsum("hid,hjd->hij", left_vals, right_vals, precision=EXACT_PRECISION), 0.0
    )


def recur(reads, rec_keys, rec_values, log_decay, learn_rate, group_gain):
    num_rows = reads.shape[0]
    num_heads = reads.shape[1] // HEAD
    blocks = num_rows // BLOCK

    def by_block(values):
        return (
            values.astype(jnp.float32).reshape(blocks, BLOCK, num_heads, HEAD).transpose(0, 2, 1, 3)
        )

    read_vals = by_block(reads)
    key_vals = by_block(rec_keys)
    value_vals = by_block(rec_values)
    decay_vals = by_block(log_decay)
    unit_key = key_vals * lax.rsqrt(jnp.sum(key_vals * key_vals, axis=-1, keepdims=True) + KEY_EPS)
    removal = -unit_key
    writing = unit_key * learn_rate.reshape(num_heads, HEAD)[None, :, None, :]
    stacked = jnp.concatenate([jnp.zeros_like(value_vals), value_vals], axis=-1)
    unit_matrix = jnp.broadcast_to(jnp.eye(HEAD, dtype=jnp.float32), (num_heads, HEAD, HEAD))
    start_pair = jnp.concatenate(
        [unit_matrix, jnp.zeros((num_heads, HEAD, HEAD), jnp.float32)], axis=1
    )
    row_iota = lax.broadcasted_iota(jnp.int32, (BLOCK, BLOCK), 0)
    col_iota = lax.broadcasted_iota(jnp.int32, (BLOCK, BLOCK), 1)
    strict = (row_iota > col_iota)[None]
    inclusive = (row_iota >= col_iota)[None]

    def block_step(state_per_block, inputs):
        read_now, key_now, removal_now, writing_now, decay_now, current_value = inputs
        cum_decay = jnp.cumsum(decay_now, axis=1)
        decay_matrix_a = removal_now * jnp.exp(cum_decay - decay_now)
        decay_matrix_b = writing_now * jnp.exp(-cum_decay)
        stacked_key_matrix = key_now * jnp.exp(-cum_decay)
        stacked_receptance = read_now * jnp.exp(cum_decay)
        m_ab = pair_table(decay_matrix_a, decay_matrix_b, strict)
        m_ak = pair_table(decay_matrix_a, stacked_key_matrix, strict)
        m_rb = pair_table(stacked_receptance, decay_matrix_b, inclusive)
        m_rk = pair_table(stacked_receptance, stacked_key_matrix, inclusive)
        right_operand = jnp.einsum(
            "bvq,bzq->bvz", decay_matrix_a, state_per_block, precision=EXACT_PRECISION
        ) + jnp.einsum("hij,hjm->him", m_ak, current_value, precision=EXACT_PRECISION)
        delta_updates = jnp.einsum(
            "hij,hjm->him", unit_inverse(m_ab), right_operand, precision=EXACT_PRECISION
        )
        block_out = (
            jnp.einsum(
                "bvq,bzq->bvz", stacked_receptance, state_per_block, precision=EXACT_PRECISION
            )
            + jnp.einsum("hij,hjm->him", m_rb, delta_updates, precision=EXACT_PRECISION)
            + jnp.einsum("hij,hjm->him", m_rk, current_value, precision=EXACT_PRECISION)
        )
        grown_state = (
            state_per_block
            + jnp.einsum("sao,sac->soc", delta_updates, decay_matrix_b, precision=EXACT_PRECISION)
            + jnp.einsum(
                "sao,sac->soc", current_value, stacked_key_matrix, precision=EXACT_PRECISION
            )
        )
        return (grown_state * jnp.exp(cum_decay[:, -1])[:, None, :], block_out)

    final_state, block_outs = lax.scan(
        block_step, start_pair, (read_vals, key_vals, removal, writing, decay_vals, stacked)
    )

    def chain(earlier, later_pair):
        moved_state = jnp.einsum(
            "hmk,hkj->hmj", earlier, later_pair[:, :HEAD], precision=EXACT_PRECISION
        )
        return moved_state + jnp.concatenate(
            [jnp.zeros_like(later_pair[:, HEAD:]), later_pair[:, HEAD:]], axis=1
        )

    carried = prefix(final_state, "sp", chain, start_pair)
    incoming = carried[:, HEAD:]
    result = block_outs[..., HEAD:] + jnp.einsum(
        "nhlm,hvm->nhlv", block_outs[..., :HEAD], incoming, precision=EXACT_PRECISION
    )
    mean_val = jnp.mean(result, axis=-1, keepdims=True)
    centered = result - mean_val
    variance = jnp.mean(centered * centered, axis=-1, keepdims=True)
    normed = (
        (centered * lax.rsqrt(variance + GROUP_EPS))
        .transpose(0, 2, 1, 3)
        .reshape(num_rows, num_heads * HEAD)
    )
    return (normed * group_gain).astype(jnp.bfloat16)


def per_device(
    tokens,
    norm_gain,
    query_w,
    key_w,
    value_w,
    recept_w,
    rec_key_w,
    rec_value_w,
    decay_down,
    decay_up,
    decay_base,
    learn_rate,
    query_gain,
    key_gain,
    sink_logit,
    group_gain,
    out_att_w,
    out_rec_w,
):
    groups = lax.axis_size(("fs", "tp"))
    own_width = tokens.shape[1]
    own_values = tokens.astype(jnp.float32)
    squares = lax.psum(jnp.sum(own_values * own_values, axis=1), ("fs", "tp"))
    gain_part = lax.dynamic_slice_in_dim(
        norm_gain, lax.axis_index(("fs", "tp")) * own_width, own_width, 0
    )
    scaled = own_values * lax.rsqrt(squares / (own_width * groups) + NORM_EPS)[:, None] * gain_part
    outgoing = scaled.astype(jnp.bfloat16)
    gathered = lax.all_gather(outgoing, ("fs", "tp"), axis=1, tiled=True)

    def rounded(sums):
        return lax.optimization_barrier(
            tuple((acc_total.astype(jnp.bfloat16) for acc_total in sums))
        )

    rec_span = recept_w.shape[1]
    decay_cols = lax.dynamic_slice_in_dim(
        decay_up, lax.axis_index(("fs", "tp")) * rec_span, rec_span, 1
    )
    decay_low = jnp.tanh(jnp.dot(gathered, decay_down, preferred_element_type=jnp.float32)).astype(
        jnp.bfloat16
    )
    decay_rate = jnp.dot(decay_low, decay_cols, preferred_element_type=jnp.float32) + jnp.repeat(
        decay_base.T, HEAD, axis=1
    )
    log_decay = -jnp.exp(decay_rate)
    pieces = (
        lax.all_gather(query_w, "sp", axis=0, tiled=True),
        lax.all_gather(key_w, "sp", axis=0, tiled=True),
        lax.all_gather(value_w, "sp", axis=0, tiled=True),
        lax.all_gather(recept_w, "sp", axis=0, tiled=True),
        lax.all_gather(rec_key_w, "sp", axis=0, tiled=True),
        lax.all_gather(rec_value_w, "sp", axis=0, tiled=True),
    )
    all_sums = tuple(
        (
            jnp.dot(gathered, weight_piece, preferred_element_type=jnp.float32)
            for weight_piece in pieces
        )
    )
    att_inputs = rounded(all_sums[:3])
    att_mix, row_lse = attend(
        att_inputs[0], att_inputs[1], att_inputs[2], query_gain, key_gain, sink_logit
    )
    rec_sums = all_sums[3:]
    rec_inputs = rounded(rec_sums)
    rec_mix = recur(rec_inputs[0], rec_inputs[1], rec_inputs[2], log_decay, learn_rate, group_gain)
    att_full, rec_full = (
        lax.all_gather(out_att_w, "sp", axis=1, tiled=True),
        lax.all_gather(out_rec_w, "sp", axis=1, tiled=True),
    )
    mixed_out = lax.psum_scatter(
        (
            jnp.dot(att_mix, att_full, preferred_element_type=jnp.float32)
            + jnp.dot(rec_mix, rec_full, preferred_element_type=jnp.float32)
        ).astype(jnp.bfloat16),
        ("fs", "tp"),
        scatter_dimension=0,
        tiled=True,
    )
    return (mixed_out, row_lse)


def general(mesh):
    in_specs = (
        P("sp", ("fs", "tp")),
        P(),
        P("sp", ("fs", "tp")),
        P("sp", ("fs", "tp")),
        P("sp", ("fs", "tp")),
        P("sp", ("fs", "tp")),
        P("sp", ("fs", "tp")),
        P("sp", ("fs", "tp")),
        P(),
        P(),
        P(("fs", "tp"), "sp"),
        P(("fs", "tp")),
        P(),
        P(),
        P(("fs", "tp")),
        P(("fs", "tp")),
        P(("fs", "tp"), "sp"),
        P(("fs", "tp"), "sp"),
    )
    out_specs = (P(("sp", "fs", "tp"), None), P(("fs", "tp"), "sp"))
    return jax.shard_map(
        per_device, mesh=mesh, in_specs=in_specs, out_specs=out_specs, check_vma=False
    )


LANES = 128
CHUNK = 64
MESH = pl.DeviceIdType.MESH


def dot(a, b):
    return jnp.dot(a, b, preferred_element_type=jnp.float32)


def dot_t(a, b, dims):
    return lax.dot_general(a, b, (dims, ((), ())), preferred_element_type=jnp.float32)


def halves(values):
    high = values.astype(jnp.bfloat16)
    return high, (values - high.astype(jnp.float32)).astype(jnp.bfloat16)


def exact(a, b, dims=((1,), (0,))):
    a_hi, a_lo = halves(a)
    b_hi, b_lo = halves(b)
    return dot_t(a_hi, b_hi, dims) + (dot_t(a_hi, b_lo, dims) + dot_t(a_lo, b_hi, dims))


def layer_kernel(n_sp, n_fs, n_tp, *refs):
    (tok, gain, recept_w, rec_key_w, rec_value_w, query_w, kv_w, out_att, out_rec) = refs[:9]
    (down, up, base, rate, q_gain, k_gain, sink, g_gain, out, lse_out) = refs[9:19]
    w_bufs = refs[19:26]
    (tok_buf, hid, halo_out, halo_in, state_out, state_in, part, part_in) = refs[26:34]
    (ward_out, ward_low, got, got_low, pair_in, pair_sum) = refs[34:40]
    (ring_send, ring_recv, chip_send, chip_recv, core_send, core_recv, ward_send, ward_recv,
     one_send, one_recv, st_send, st_recv, red_send, red_recv, pair_send, pair_recv) = refs[40:]
    weights = (recept_w, rec_key_w, rec_value_w, query_w, kv_w, out_att, out_rec)
    groups = n_fs * n_tp
    place = lax.axis_index("sp")
    own = lax.axis_index("fs") * n_tp + lax.axis_index("tp")
    rows = tok.shape[0]

    def peer(step):
        other = lax.rem(own + step, groups)
        return {"fs": lax.div(other, n_tp), "tp": lax.rem(other, n_tp)}

    barrier = pltpu.get_barrier_semaphore()
    for step in range(1, groups):
        pl.semaphore_signal(barrier, inc=1, device_id=peer(step), device_id_type=MESH)
    for step in range(1, n_sp):
        pl.semaphore_signal(
            barrier, inc=1, device_id={"sp": lax.rem(place + step, n_sp)}, device_id_type=MESH
        )
    pl.semaphore_wait(barrier, groups - 1 + n_sp - 1)

    def hop(item, way, step):
        sign = 1 if way == 0 else -1
        src = weights[item] if step == 0 else w_bufs[item].at[lax.rem(place - sign * step + n_sp, n_sp)]
        return pltpu.make_async_remote_copy(
            src_ref=src,
            dst_ref=w_bufs[item].at[lax.rem(place - sign * step + n_sp, n_sp)],
            send_sem=ring_send.at[item, way, step],
            recv_sem=ring_recv.at[item, way, step],
            device_id={"sp": lax.rem(place + sign + n_sp, n_sp)},
            device_id_type=MESH,
        )

    def inner(at):
        return (at >= 1) & (at <= n_sp - 2)

    inside = inner(place)
    outside = ~inside
    helps = inside & ((place == 1) | (place == n_sp - 2))
    partner = jnp.where(
        place == 0, 1, jnp.where(place == n_sp - 1, n_sp - 2, jnp.where(place == 1, 0, n_sp - 1))
    )
    inputs = 5

    def sends(item, way, step):
        if way == 0:
            base_case, to = (place >= step) & (place + 1 < n_sp), place + 1
        else:
            base_case, to = (place + step < n_sp) & (place >= 1), place - 1
        return base_case & inner(to) if item < inputs else base_case

    def takes(item, way, step):
        base_case = place >= step + 1 if way == 0 else place + step + 1 < n_sp
        return base_case & inside if item < inputs else base_case

    def start(items, step, to_inner):
        for item in items:
            for way in (0, 1):
                to = inner(place + (1 if way == 0 else -1))

                @pl.when(sends(item, way, step) & (to if to_inner else ~to))
                def _():
                    hop(item, way, step).start()

    def sent(item, step):
        for way in (0, 1):

            @pl.when(sends(item, way, step))
            def _():
                hop(item, way, step).wait_send()

    def relay(items, step, from_inner):
        for item in items:
            for way in (0, 1):
                origin = inner(place - (1 if way == 0 else -1))
                mine = inside & (origin if from_inner else ~origin)

                @pl.when(takes(item, way, step) & mine)
                def _():
                    hop(item, way, step).wait_recv()

                if step + 1 < n_sp - 1:

                    @pl.when(sends(item, way, step + 1) & mine)
                    def _():
                        hop(item, way, step + 1).start()

    rec_items, att_items, out_items = (0, 1, 2), (3, 4), (5, 6)

    def ward_tok():
        return pltpu.make_async_remote_copy(
            src_ref=tok, dst_ref=tok_buf.at[1, own], send_sem=ward_send.at[0],
            recv_sem=ward_recv.at[0], device_id={"sp": partner}, device_id_type=MESH,
        )

    fs_at, tp_at = lax.axis_index("fs"), lax.axis_index("tp")

    def chip_copy(which, step):
        return pltpu.make_async_remote_copy(
            src_ref=tok if which == 0 else tok_buf.at[1, own], dst_ref=tok_buf.at[which, own],
            send_sem=chip_send.at[which, step - 1], recv_sem=chip_recv.at[which, step - 1],
            device_id={"fs": lax.rem(fs_at + step, n_fs)}, device_id_type=MESH,
        )

    def core_copy(which, step, turn):
        slot = lax.rem(fs_at - step + n_fs, n_fs) * n_tp + tp_at
        return pltpu.make_async_remote_copy(
            src_ref=tok if which == 0 and step == 0 else tok_buf.at[which, slot],
            dst_ref=tok_buf.at[which, slot],
            send_sem=core_send.at[which, step, turn - 1], recv_sem=core_recv.at[which, step, turn - 1],
            device_id={"tp": lax.rem(tp_at + turn, n_tp)}, device_id_type=MESH,
        )

    def to_chips(which):
        for step in range(1, n_fs):
            chip_copy(which, step).start()
        for turn in range(1, n_tp):
            core_copy(which, 0, turn).start()

    def to_cores(which):
        for step in range(1, n_fs):
            chip_copy(which, step).wait_recv()
            for turn in range(1, n_tp):
                core_copy(which, step, turn).start()

    def all_tokens(which):
        for step in range(n_fs):
            for turn in range(1, n_tp):
                core_copy(which, step, turn).wait_recv()

    width = tok.shape[1]

    def input_norm(which):
        squares = jnp.zeros((rows, 1), jnp.float32)
        for group in range(groups):
            values = tok_buf[which, group].astype(jnp.float32)
            squares = squares + jnp.sum(values * values, axis=1, keepdims=True)
        inv_rms = lax.rsqrt(squares / (width * groups) + NORM_EPS)
        for group in range(groups):
            cut = slice(group * width, (group + 1) * width)
            hid[which, :, cut] = (
                tok_buf[which, group].astype(jnp.float32) * inv_rms * gain[:, cut]
            ).astype(jnp.bfloat16)

    def project(which, item):
        buf = w_bufs[item]
        flat = buf[...].reshape(buf.shape[0] * buf.shape[1], buf.shape[2])
        return dot(hid[which], flat).astype(jnp.bfloat16)

    def low_rank(which):
        return jnp.tanh(dot(hid[which], down[...])).astype(jnp.bfloat16)

    def ward_copy(item):
        source, target = (ward_low, got_low) if item == inputs else (ward_out.at[item], got.at[item])
        return pltpu.make_async_remote_copy(
            src_ref=source, dst_ref=target, send_sem=ward_send.at[1 + item],
            recv_sem=ward_recv.at[1 + item], device_id={"sp": partner}, device_id_type=MESH,
        )

    @pl.when(outside)
    def _():
        ward_tok().start()

    @pl.when(inside)
    def _():
        to_chips(0)

    start(rec_items, 0, True)
    start(out_items, 0, False)

    @pl.when(outside)
    def _():
        start(att_items, 0, True)
        start(out_items, 0, True)

    tok_buf[0, own] = tok[...]
    for item in range(len(weights)):
        w_bufs[item][place] = weights[item][...]

    @pl.when(place == 0)
    def _():
        halo_in[...] = jnp.zeros_like(halo_in)

    @pl.when(helps)
    def _():
        ward_tok().wait_recv()
        to_chips(1)

    @pl.when(inside)
    def _():
        to_cores(0)

    relay(rec_items[:2], 0, False)

    @pl.when(inside)
    def _():
        all_tokens(0)
        input_norm(0)

    relay(rec_items[2:], 0, False)
    relay(rec_items, 0, True)

    @pl.when(inside)
    def _():
        start(att_items, 0, True)

    @pl.when(helps)
    def _():
        to_cores(1)
        all_tokens(1)
        input_norm(1)

    relay(att_items, 0, False)

    @pl.when(inside)
    def _():
        start(out_items, 0, True)

    for step in range(1, n_sp - 2):
        relay(rec_items, step, True)

    @pl.when(helps)
    def _():
        for item in rec_items:
            ward_out[item] = project(1, item)
        ward_low[...] = low_rank(1)

    @pl.when(inside)
    def _():
        got_low[...] = low_rank(0)

    @pl.when(helps)
    def _():
        for item in rec_items + (inputs,):
            ward_copy(item).start()

    @pl.when(inside)
    def _():
        for item in rec_items:
            got[item] = project(0, item)

    @pl.when(outside)
    def _():
        for item in rec_items + (inputs,):
            ward_copy(item).wait_recv()

    span = recept_w.shape[1]
    up_cols = up[:, pl.ds(pl.multiple_of(own * span, LANES), span)]
    log_decay = -jnp.exp(dot(got_low[...], up_cols) + base[...])
    reads = got[0].astype(jnp.float32)
    keys = got[1].astype(jnp.float32)
    vals = got[2].astype(jnp.float32)

    chunks = rows // CHUNK
    row_at = lax.broadcasted_iota(jnp.int32, (rows, rows), 0)
    col_at = lax.broadcasted_iota(jnp.int32, (rows, rows), 1)
    same = lax.div(row_at, CHUNK) == lax.div(col_at, CHUNK)
    inclusive = same & (row_at >= col_at)
    strict = same & (row_at > col_at)
    ones = jnp.where(inclusive, 1.0, 0.0).astype(jnp.bfloat16)
    ld_hi, ld_lo = halves(log_decay)
    ld_rest = (log_decay - ld_hi.astype(jnp.float32) - ld_lo.astype(jnp.float32)).astype(jnp.bfloat16)
    cum = dot(ones, ld_hi) + (dot(ones, ld_lo) + dot(ones, ld_rest))
    cum_c = cum.reshape(chunks, CHUNK, span)
    middle = cum_c[:, CHUNK // 2 - 1 : CHUNK // 2, :]
    last = cum_c[:, CHUNK - 1 : CHUNK, :]
    rel = (cum_c - middle).reshape(rows, span)
    to_end = jnp.exp(last - cum_c).reshape(rows, span)
    eye = jnp.where(
        lax.broadcasted_iota(jnp.int32, (HEAD, HEAD), 0) == lax.broadcasted_iota(jnp.int32, (HEAD, HEAD), 1),
        1.0, 0.0,
    )
    big_eye = jnp.where(row_at == col_at, 1.0, 0.0)
    zeros = jnp.zeros((HEAD, HEAD), jnp.float32)
    rec_heads = span // HEAD
    from_start, own_part = [], []
    for head in range(rec_heads):
        at = slice(head * HEAD, (head + 1) * HEAD)
        k, v, r = keys[:, at], vals[:, at], reads[:, at]
        unit = k * lax.rsqrt(jnp.sum(k * k, axis=1, keepdims=True) + KEY_EPS)
        write = unit * rate[:, at]
        before = cum[:, at] - log_decay[:, at]
        up_rel, down_rel = jnp.exp(rel[:, at]), jnp.exp(-rel[:, at])
        left = jnp.concatenate([-unit * jnp.exp(rel[:, at] - log_decay[:, at]), r * up_rel], axis=0)
        right = jnp.concatenate([write * down_rel, k * down_rel], axis=0)
        table = exact(left, right, ((1,), (1,)))
        m_ab = jnp.where(strict, table[:rows, :rows], 0.0)
        m_ak = jnp.where(strict, table[:rows, rows:], 0.0)
        m_rb = jnp.where(inclusive, table[rows:, :rows], 0.0)
        m_rk = jnp.where(inclusive, table[rows:, rows:], 0.0)
        inverse, power = big_eye + m_ab, m_ab
        for _ in range(CHUNK.bit_length() - 2):
            power = exact(power, power)
            inverse = inverse + exact(inverse, power)
        pu = exact(inverse, jnp.concatenate([-unit * jnp.exp(before), exact(m_ak, v)], axis=1))
        mixed_pu = exact(m_rb, pu)
        given = r * jnp.exp(cum[:, at]) + mixed_pu[:, :HEAD]
        offset = mixed_pu[:, HEAD:] + exact(m_rk, v)
        b_end, k_end = write * to_end[:, at], k * to_end[:, at]
        pair = jnp.concatenate([eye, zeros], axis=1)
        reach = []
        for chunk in range(chunks):
            cut = slice(chunk * CHUNK, (chunk + 1) * CHUNK)
            reach.append(exact(given[cut], pair))
            step_map = exact(b_end[cut], pu[cut], ((0,), (0,)))
            turn = step_map[:, :HEAD] + eye * jnp.exp(last[chunk][:, at])
            grown = step_map[:, HEAD:] + exact(k_end[cut], v[cut], ((0,), (0,)))
            pair = exact(turn, pair) + jnp.concatenate([zeros, grown], axis=1)
        reach = jnp.concatenate(reach, axis=0)
        from_start.append(reach[:, :HEAD])
        own_part.append(reach[:, HEAD:] + offset)
        state_out[head] = pair.astype(jnp.bfloat16)
        if head == 0:
            relay(out_items, 0, False)

    def state_copy(step):
        return pltpu.make_async_remote_copy(
            src_ref=state_out, dst_ref=state_in.at[place], send_sem=st_send.at[step - 1],
            recv_sem=st_recv.at[step - 1], device_id={"sp": lax.rem(place + step, n_sp)},
            device_id_type=MESH,
        )

    for step in range(n_sp - 2):
        relay(att_items, step, True)
    for step in range(1, n_sp):
        @pl.when(place + step < n_sp)
        def _():
            state_copy(step).start()

    @pl.when(helps)
    def _():
        for item in att_items:
            ward_out[item] = project(1, item)

    @pl.when(inside)
    def _():
        for item in att_items:
            got[item] = project(0, item)

    @pl.when(helps)
    def _():
        for item in att_items:
            ward_copy(item).start()

    relay(out_items, 0, True)

    @pl.when(outside)
    def _():
        for item in att_items:
            ward_copy(item).wait_recv()

    q_all = got[3].astype(jnp.float32)
    kv_all = got[4].astype(jnp.float32)
    kv_heads = kv_all.shape[1] // (2 * HEAD)
    q_heads = q_all.shape[1] // HEAD
    share = q_heads // kv_heads

    def normed(values, gain_ref):
        mean_sq = jnp.mean(values * values, axis=1, keepdims=True)
        return (values * lax.rsqrt(mean_sq + NORM_EPS) * gain_ref[...]).astype(jnp.bfloat16)

    key_n = [normed(kv_all[:, h * HEAD : (h + 1) * HEAD], k_gain) for h in range(kv_heads)]
    value_n = [
        kv_all[:, (kv_heads + h) * HEAD : (kv_heads + h + 1) * HEAD].astype(jnp.bfloat16)
        for h in range(kv_heads)
    ]
    halo_out[...] = jnp.concatenate([x[rows - WINDOW :] for x in key_n + value_n], axis=1)
    query_n = [normed(q_all[:, h * HEAD : (h + 1) * HEAD], q_gain) for h in range(q_heads)]

    def halo_copy():
        return pltpu.make_async_remote_copy(
            src_ref=halo_out, dst_ref=halo_in, send_sem=one_send.at[0], recv_sem=one_recv.at[0],
            device_id={"sp": lax.rem(place + 1, n_sp)}, device_id_type=MESH,
        )

    @pl.when(place + 1 < n_sp)
    def _():
        halo_copy().start()

    blocks = rows // WINDOW
    lag = (
        lax.broadcasted_iota(jnp.int32, (WINDOW, 2 * WINDOW), 0)
        + WINDOW
        - lax.broadcasted_iota(jnp.int32, (WINDOW, 2 * WINDOW), 1)
    )
    key_col = lax.broadcasted_iota(jnp.int32, (WINDOW, 2 * WINDOW), 1)
    mixes = [[None] * q_heads for _ in range(blocks)]

    def attend_block(block, band_keys, band_values):
        allowed = (lag >= 0) & (lag < WINDOW)
        if block == 0:
            allowed = allowed & (key_col + (place * blocks - 1) * WINDOW >= 0)
        cut = slice(block * WINDOW, (block + 1) * WINDOW)
        for h in range(q_heads):
            top_sink = sink[0, h]
            scores = dot_t(query_n[h][cut], band_keys[h // share], ((1,), (1,))) * (1.0 / math.sqrt(HEAD))
            masked = jnp.where(allowed, scores, -jnp.inf)
            top = jnp.maximum(jnp.max(masked, axis=1, keepdims=True), top_sink)
            weight = jnp.where(allowed, jnp.exp(masked - top), 0.0)
            total = jnp.sum(weight, axis=1, keepdims=True) + jnp.exp(top_sink - top)
            spread = jnp.broadcast_to(top + jnp.log(total), (WINDOW, LANES)).T
            lse_out[h : h + 1, cut] = spread[0:1]
            probs = (weight / total).astype(jnp.bfloat16)
            mixes[block][h] = dot(probs, band_values[h // share]).astype(jnp.bfloat16)

    for block in range(1, blocks):
        band = slice((block - 1) * WINDOW, (block + 1) * WINDOW)
        attend_block(block, [x[band] for x in key_n], [x[band] for x in value_n])

    @pl.when(place >= 1)
    def _():
        halo_copy().wait_recv()

    halo = halo_in[...]
    before_k = [halo[:, h * HEAD : (h + 1) * HEAD] for h in range(kv_heads)]
    before_v = [halo[:, (kv_heads + h) * HEAD : (kv_heads + h + 1) * HEAD] for h in range(kv_heads)]
    attend_block(
        0,
        [jnp.concatenate([b, x[:WINDOW]], axis=0) for b, x in zip(before_k, key_n)],
        [jnp.concatenate([b, x[:WINDOW]], axis=0) for b, x in zip(before_v, value_n)],
    )
    att_mix = jnp.concatenate([jnp.concatenate(line, axis=1) for line in mixes], axis=0)
    for step in range(1, n_sp - 2):
        relay(out_items, step, True)

    @pl.when(outside)
    def _():
        for item in out_items:
            for step in range(n_sp - 1):
                for way in (0, 1):

                    @pl.when(takes(item, way, step))
                    def _():
                        hop(item, way, step).wait_recv()

    for step in range(1, n_sp):
        @pl.when(place >= step)
        def _():
            state_copy(step).wait_recv()
    rec_parts = []
    for head in range(rec_heads):
        state = zeros
        for k in range(n_sp - 1):
            pair = state_in[k, head].astype(jnp.float32)
            moved = exact(pair[:, :HEAD], state) + pair[:, HEAD:]
            state = jnp.where(place > k, moved, state)
        result = own_part[head] + exact(from_start[head], state)
        mean_val = jnp.mean(result, axis=1, keepdims=True)
        centered = result - mean_val
        variance = jnp.mean(centered * centered, axis=1, keepdims=True)
        at = slice(head * HEAD, (head + 1) * HEAD)
        rec_parts.append((centered * lax.rsqrt(variance + GROUP_EPS) * g_gain[:, at]).astype(jnp.bfloat16))
    rec_mix = jnp.concatenate(rec_parts, axis=1)

    cols = out_att.shape[1]
    few = rows // groups
    for k in range(n_sp):
        block = (dot(att_mix, w_bufs[5][k]) + dot(rec_mix, w_bufs[6][k])).astype(jnp.bfloat16)
        for group in range(groups):
            part[group % n_tp, group // n_tp, :, k * cols : (k + 1) * cols] = block[
                group * few : (group + 1) * few
            ]

    def pair_copy(step, turn):
        to = lax.rem(tp_at + turn, n_tp)
        chip = lax.rem(fs_at + step, n_fs)
        return pltpu.make_async_remote_copy(
            src_ref=part.at[to, chip], dst_ref=pair_in.at[turn - 1, step],
            send_sem=pair_send.at[step, turn - 1], recv_sem=pair_recv.at[step, turn - 1],
            device_id={"tp": to}, device_id_type=MESH,
        )

    def red_copy(step):
        return pltpu.make_async_remote_copy(
            src_ref=pair_sum.at[step - 1], dst_ref=part_in.at[step - 1],
            send_sem=red_send.at[step - 1], recv_sem=red_recv.at[step - 1],
            device_id={"fs": lax.rem(fs_at + step, n_fs)}, device_id_type=MESH,
        )

    def chip_total(step):
        value = part[tp_at, lax.rem(fs_at + step, n_fs)].astype(jnp.float32)
        for turn in range(1, n_tp):
            pair_copy(step, turn).wait_recv()
            value = value + pair_in[turn - 1, step].astype(jnp.float32)
        return value

    order = [*range(n_fs - 1, 0, -1), 0]
    for step in order:
        for turn in range(1, n_tp):
            pair_copy(step, turn).start()
    for step in order[:-1]:
        pair_sum[step - 1] = chip_total(step).astype(jnp.bfloat16)
        red_copy(step).start()
    @pl.when(outside)
    def _():
        ward_tok().wait_send()

    def tokens_sent(which):
        for step in range(1, n_fs):
            chip_copy(which, step).wait_send()
        for step in range(n_fs):
            for turn in range(1, n_tp):
                core_copy(which, step, turn).wait_send()

    @pl.when(inside)
    def _():
        tokens_sent(0)

    @pl.when(helps)
    def _():
        tokens_sent(1)
        for item in range(inputs + 1):
            ward_copy(item).wait_send()

    for item in range(len(weights)):
        for step in range(n_sp - 1):
            sent(item, step)
    for step in range(1, n_sp):
        @pl.when(place + step < n_sp)
        def _():
            state_copy(step).wait_send()

    @pl.when(place + 1 < n_sp)
    def _():
        halo_copy().wait_send()

    total = chip_total(0)
    for step in order[:-1]:
        red_copy(step).wait_recv()
        total = total + part_in[step - 1].astype(jnp.float32)
    out[...] = total.astype(jnp.bfloat16)
    for step in range(n_fs):
        for turn in range(1, n_tp):
            pair_copy(step, turn).wait_send()
        if step:
            red_copy(step).wait_send()


def in_kernel(
    n_sp, n_fs, n_tp,
    tokens, norm_gain, query_w, key_w, value_w, recept_w, rec_key_w, rec_value_w,
    decay_down, decay_up, decay_base, learn_rate, query_gain, key_gain, sink_logit,
    group_gain, out_att_w, out_rec_w,
):
    groups = n_fs * n_tp
    rows, width = tokens.shape
    rec_span = recept_w.shape[1]
    model = width * groups
    base = jnp.repeat(decay_base.T, HEAD, axis=1)
    kv_w = jnp.concatenate([key_w, value_w], axis=1)
    weights = (recept_w, rec_key_w, rec_value_w, query_w, kv_w, out_att_w, out_rec_w)
    vmem = pl.BlockSpec(memory_space=pltpu.VMEM)
    smem = pl.BlockSpec(memory_space=pltpu.SMEM)
    bf16 = jnp.bfloat16
    heads = rec_span // HEAD
    dma = pltpu.SemaphoreType.DMA
    scratch = [pltpu.VMEM((n_sp, *w.shape), bf16) for w in weights] + [
        pltpu.VMEM((2, groups, rows, width), bf16),
        pltpu.VMEM((2, rows, model), bf16),
        pltpu.VMEM((WINDOW, kv_w.shape[1]), bf16),
        pltpu.VMEM((WINDOW, kv_w.shape[1]), bf16),
        pltpu.VMEM((heads, HEAD, 2 * HEAD), bf16),
        pltpu.VMEM((n_sp, heads, HEAD, 2 * HEAD), bf16),
        pltpu.VMEM((n_tp, n_fs, rows // groups, model), bf16),
        pltpu.VMEM((n_fs - 1, rows // groups, model), bf16),
        pltpu.VMEM((5, rows, rec_span), bf16),
        pltpu.VMEM((rows, decay_down.shape[1]), bf16),
        pltpu.VMEM((5, rows, rec_span), bf16),
        pltpu.VMEM((rows, decay_down.shape[1]), bf16),
        pltpu.VMEM((n_tp - 1, n_fs, rows // groups, model), bf16),
        pltpu.VMEM((n_fs - 1, rows // groups, model), bf16),
        dma((len(weights), 2, n_sp - 1)),
        dma((len(weights), 2, n_sp - 1)),
        dma((2, n_fs - 1)),
        dma((2, n_fs - 1)),
        dma((2, n_fs, n_tp - 1)),
        dma((2, n_fs, n_tp - 1)),
        dma((7,)),
        dma((7,)),
        dma((1,)),
        dma((1,)),
        dma((n_sp - 1,)),
        dma((n_sp - 1,)),
        dma((n_fs - 1,)),
        dma((n_fs - 1,)),
        dma((n_fs, n_tp - 1)),
        dma((n_fs, n_tp - 1)),
    ]
    return pl.pallas_call(
        functools.partial(layer_kernel, n_sp, n_fs, n_tp),
        out_shape=(
            jax.ShapeDtypeStruct((rows // groups, model), bf16),
            jax.ShapeDtypeStruct((sink_logit.shape[0], rows), jnp.float32),
        ),
        in_specs=[vmem] * 15 + [smem] + [vmem],
        out_specs=(vmem, vmem),
        scratch_shapes=scratch,
        compiler_params=pltpu.CompilerParams(
            collective_id=0, has_side_effects=True, vmem_limit_bytes=60 * 1024 * 1024
        ),
    )(
        tokens, norm_gain[None], *weights, decay_down, decay_up, base, learn_rate[None],
        query_gain[None], key_gain[None], sink_logit[None], group_gain[None],
    )


def solution(mesh):
    n_sp, n_fs, n_tp = (mesh.shape[name] for name in ("sp", "fs", "tp"))
    plain = general(mesh)

    def layer(*arrays):
        if (arrays[-1].shape[1] // n_sp) % LANES or n_sp > LANES // 8 or n_sp < 4:
            return plain(*arrays)
        in_specs = (
            P("sp", ("fs", "tp")),
            P(),
            P("sp", ("fs", "tp")),
            P("sp", ("fs", "tp")),
            P("sp", ("fs", "tp")),
            P("sp", ("fs", "tp")),
            P("sp", ("fs", "tp")),
            P("sp", ("fs", "tp")),
            P(),
            P(),
            P(("fs", "tp"), "sp"),
            P(("fs", "tp")),
            P(),
            P(),
            P(("fs", "tp")),
            P(("fs", "tp")),
            P(("fs", "tp"), "sp"),
            P(("fs", "tp"), "sp"),
        )
        out_specs = (P(("sp", "fs", "tp"), None), P(("fs", "tp"), "sp"))
        return jax.shard_map(
            functools.partial(in_kernel, n_sp, n_fs, n_tp),
            mesh=mesh, in_specs=in_specs, out_specs=out_specs, check_vma=False,
        )(*arrays)

    return layer
```
